32 devices in a mesh: kv: 16 (over z, y, core), tp: 2 (over x).
Axes of the slice: x: 2, y: 2, z: 4, core: 2. Of those that a mesh axis runs over, the one named last changes fastest.
Arguments:
- tokens: bfloat16 [12, 2048], replicated, may hold values from -6 to 6
- w_query: bfloat16 [2048, 2048], P(None, 'tp'), may hold values from -0.125 to 0.125
- w_key: bfloat16 [2048, 512], P(None, 'tp'), may hold values from -0.125 to 0.125
- w_value: bfloat16 [2048, 512], P(None, 'tp'), may hold values from -0.125 to 0.125
- w_gate: bfloat16 [2048, 32], replicated, may hold values from -0.125 to 0.125
- w_out: bfloat16 [2048, 2048], P(None, 'tp'), may hold values from -0.125 to 0.125
- key_cache: bfloat16 [12, 4096, 512], P(None, 'kv', 'tp'), may hold values from -270 to 270
- value_cache: bfloat16 [12, 4096, 512], P(None, 'kv', 'tp'), may hold values from -6 to 6
- key_summary: bfloat16 [12, 256, 512], P(None, 'kv', 'tp'), may hold values from -260 to 260
- value_summary: bfloat16 [12, 256, 512], P(None, 'kv', 'tp'), may hold values from -6 to 6
- lengths: int32 [12], replicated, may hold values from 16 to 4096, as said below
- chosen: int32 [12, 4, 128], P(None, 'tp', 'kv'), may hold values from 0 to 1, as said below
Outputs:
- attended: bfloat16 [12, 2048], P(None, 'tp')
The draws below stay inside these ranges and needn't reach their ends.
Inputs may be any that keep to these rules, and one draw needn't show every extreme that they name: `lengths`: at least one sequence has length 4096. `chosen`: for each sequence s and key head, exactly min(16, live blocks) entries are 1, the live blocks being those that hold a position below lengths[s]; block 0, block 64 when it is live, and the block holding position lengths[s] - 1 are among them, and no block beyond is.
All inputs are finite; a program needn't handle non-finite values.
Results may differ from the reference program's by a relative error of at most 0.012.
Values may be sent and summed in bfloat16 or wider, within the bound.
A program may use at most 64 MiB of HBM per device.

```python
import math
import jax
import jax.numpy as jnp
from jax import lax

D = 2048
HEADS = 16
GROUPS = 4
HDIM = 128
SB = 32
CB = 16
NSEL = 16
BLK_DEV = 8
SEQS = 12
CACHE = 4096
NCMP = 256
NBLK = 128


def planted_keys(key, dims_shape, middle_rows):
    keys_a, keys_b, keys_c, keys_d = jax.random.split(key, 4)
    seq_total = dims_shape[0]
    row_total = dims_shape[1]
    width = dims_shape[2]
    group_total = width // HDIM
    noise = jnp.clip(jax.random.normal(keys_a, dims_shape, jnp.float32), -6.0, 6.0)
    row_index = jnp.arange(row_total)[None, :, None]
    middle = (row_index >= row_total // 2) & (row_index < row_total // 2 + middle_rows)
    noise = noise * jnp.where(middle, 3.0, 1.0)
    forced = (jnp.arange(seq_total)[:, None, None] == 0) & (jnp.arange(group_total)[None, None, :] == 0)
    planted = (jax.random.randint(keys_b, (seq_total, 1, group_total), 0, 4) == 0) | forced
    strength = jnp.exp(jax.random.uniform(keys_c, (seq_total, 1, group_total), jnp.float32, math.log(100.0), math.log(250.0)))
    strength = jnp.repeat(jnp.where(planted, strength, 0.0), HDIM, axis=2)
    signs = jnp.where(jax.random.randint(keys_d, (seq_total, 1, width), 0, 2) == 0, -1.0, 1.0)
    return (noise + signs * strength).astype(jnp.bfloat16)


def draw_key_cache(key, part):
    return planted_keys(jax.random.fold_in(key, 21), (SEQS, CACHE, GROUPS * HDIM), SB * BLK_DEV)


def draw_key_summary(key, part):
    return planted_keys(jax.random.fold_in(key, 22), (SEQS, NCMP, GROUPS * HDIM), 0)


def make_lengths(key):
    stream = jax.random.fold_in(key, 11)
    keys_a, keys_b, keys_c, keys_d = jax.random.split(stream, 4)
    span_top = CACHE - CB + 1
    shortest = jnp.minimum(jax.random.randint(keys_a, (SEQS,), 0, span_top), jax.random.randint(keys_b, (SEQS,), 0, span_top))
    shortest = jnp.minimum(shortest, jax.random.randint(keys_c, (SEQS,), 0, span_top))
    longest = jax.random.randint(keys_d, (), 0, SEQS)
    result = jnp.where(jnp.arange(SEQS) == longest, CACHE, CB + shortest)
    return result.astype(jnp.int32)


def draw_lengths(key, part):
    return make_lengths(key)


def draw_chosen(key, part):
    lengths = make_lengths(key)
    live_blocks = (lengths + SB - 1) // SB
    blocks = jnp.arange(NBLK, dtype=jnp.int32)
    raw_scores = jax.random.randint(jax.random.fold_in(key, 12), (SEQS, GROUPS, NBLK), 0, 65536)
    ranked = raw_scores // (1 + 4 * blocks // NBLK) * NBLK + blocks
    alive = blocks[None, None, :] < live_blocks[:, None, None]
    forced = (blocks == 0)[None, None, :] | (blocks[None, None, :] == (live_blocks - 1)[:, None, None])
    forced = forced | (blocks == NBLK // 2)[None, None, :] & alive
    ranked = jnp.where(forced, (1 << 30) + blocks, jnp.where(alive, ranked, -1 - blocks))
    _, picked = lax.top_k(ranked, NSEL)
    hit_any = jnp.any(picked[..., None] == blocks, axis=-2)
    return (hit_any & alive).astype(jnp.int32)


def levels(key, extent, cuts, smallest, top_value):
    def one(axis_at, shards_of):
        draws = jax.random.uniform(jax.random.fold_in(jax.random.fold_in(key, 6), axis_at), (shards_of,), jnp.float32, smallest / len(cuts), top_value / len(cuts))
        return jnp.repeat(jnp.exp(draws), extent[axis_at] // shards_of).reshape((-1,) + (1,) * (len(extent) - axis_at - 1))

    loudness = one(*cuts[0])
    for cut in cuts[1:]:
        loudness = loudness * one(*cut)
    return loudness


def scatter_about(rng, shape, deviation, bound, cuts=(), held_as=jnp.bfloat16):
    level = levels(rng, shape, cuts, -0.22, 0.18) if cuts else 1.0
    values = jax.random.normal(rng, shape, jnp.float32) * deviation * level
    return jnp.minimum(jnp.maximum(values, -bound), bound).astype(held_as)


def setup_inputs(seed: int = 0) -> dict:
    streams_of = jax.random.split(jax.random.key(seed), 13)
    tokens = scatter_about(streams_of[0], (SEQS, D), 1.0, 6.0)
    w_query = scatter_about(streams_of[1], (D, HEADS * HDIM), D ** -0.5, 0.125, ((1, 2),))
    w_key = scatter_about(streams_of[2], (D, GROUPS * HDIM), D ** -0.5, 0.125, ((1, 2),))
    w_value = scatter_about(streams_of[3], (D, GROUPS * HDIM), D ** -0.5, 0.125, ((1, 2),))
    w_gate = scatter_about(streams_of[4], (D, 2 * HEADS), D ** -0.5, 0.125)
    w_out = scatter_about(streams_of[5], (HEADS * HDIM, D), (HEADS * HDIM) ** -0.5, 0.125, ((1, 2),))
    key_cache = draw_key_cache(jax.random.fold_in(streams_of[12], 71), 0)
    value_cache = scatter_about(streams_of[7], (SEQS, CACHE, GROUPS * HDIM), 1.0, 6.0, ((1, 16), (2, 2)))
    key_summary = draw_key_summary(jax.random.fold_in(streams_of[12], 71), 0)
    value_summary = scatter_about(streams_of[9], (SEQS, NCMP, GROUPS * HDIM), 1.0, 6.0, ((1, 16), (2, 2)))
    lengths = draw_lengths(jax.random.fold_in(streams_of[12], 71), 0)
    chosen = draw_chosen(jax.random.fold_in(streams_of[12], 71), 0)
    return {"tokens": tokens, "w_query": w_query, "w_key": w_key, "w_value": w_value, "w_gate": w_gate, "w_out": w_out, "key_cache": key_cache, "value_cache": value_cache, "key_summary": key_summary, "value_summary": value_summary, "lengths": lengths, "chosen": chosen}


neg_fill = -1e30


def one_sequence(inputs):
    grouped, sum_keys, sum_values, sel_keys, sel_values, new_key, new_value, length, picked, gate_pair = inputs
    score_scale = HDIM ** -0.5
    sum_keys = sum_keys.astype(jnp.float32)
    sum_values = sum_values.astype(jnp.float32)
    sel_keys = sel_keys.astype(jnp.float32)
    sel_values = sel_values.astype(jnp.float32)
    new_key = new_key.astype(jnp.float32)
    new_value = new_value.astype(jnp.float32)
    live_sum = ((jnp.arange(NCMP) + 1) * CB <= length)[None, None, :]
    sum_scores = jnp.einsum("grd,ngd->grn", grouped, sum_keys) * score_scale
    sum_scores = jnp.where(live_sum, sum_scores, neg_fill)
    sum_peak = jnp.max(sum_scores, axis=-1, keepdims=True)
    sum_weights = jnp.where(live_sum, jnp.exp(sum_scores - sum_peak), 0.0)
    compressed = jnp.einsum("grn,ngd->grd", sum_weights, sum_values) / jnp.sum(sum_weights, axis=-1, keepdims=True)
    position = jnp.arange(CACHE)
    block_live = jnp.repeat(picked, SB, axis=1) != 0
    live_sel = (block_live & (position < length)[None, :])[:, None, :]
    sel_scores = jnp.einsum("grd,pgd->grp", grouped, sel_keys) * score_scale
    sel_scores = jnp.where(live_sel, sel_scores, neg_fill)
    own_score = jnp.sum(grouped * new_key[:, None, :], axis=-1) * score_scale
    peak_all = jnp.maximum(jnp.max(sel_scores, axis=-1), own_score)
    weights = jnp.where(live_sel, jnp.exp(sel_scores - peak_all[..., None]), 0.0)
    own_weight = jnp.exp(own_score - peak_all)
    numer = jnp.einsum("grp,pgd->grd", weights, sel_values) + own_weight[..., None] * new_value[:, None, :]
    selected = numer / (jnp.sum(weights, axis=-1) + own_weight)[..., None]
    mixed_heads = gate_pair[..., 0:1] * compressed + gate_pair[..., 1:2] * selected
    return mixed_heads.reshape(-1).astype(jnp.bfloat16)


def reference(tokens, w_query, w_key, w_value, w_gate, w_out, key_cache, value_cache, key_summary, value_summary, lengths, chosen):
    per_group = HEADS // GROUPS
    queries = jnp.dot(tokens, w_query, preferred_element_type=jnp.float32).astype(jnp.bfloat16)
    new_keys = jnp.dot(tokens, w_key, preferred_element_type=jnp.float32).astype(jnp.bfloat16)
    new_values = jnp.dot(tokens, w_value, preferred_element_type=jnp.float32).astype(jnp.bfloat16)
    gate_vals = jax.nn.sigmoid(jnp.dot(tokens, w_gate, preferred_element_type=jnp.float32))
    gate_vals = gate_vals.reshape(SEQS, GROUPS, per_group, 2)
    grouped = queries.astype(jnp.float32).reshape(SEQS, GROUPS, per_group, HDIM)
    mixed_all = lax.map(one_sequence, (
        grouped,
        key_summary.reshape(SEQS, NCMP, GROUPS, HDIM),
        value_summary.reshape(SEQS, NCMP, GROUPS, HDIM),
        key_cache.reshape(SEQS, CACHE, GROUPS, HDIM),
        value_cache.reshape(SEQS, CACHE, GROUPS, HDIM),
        new_keys.reshape(SEQS, GROUPS, HDIM),
        new_values.reshape(SEQS, GROUPS, HDIM),
        lengths,
        chosen,
        gate_vals))
    return jnp.dot(mixed_all, w_out, preferred_element_type=jnp.float32).astype(jnp.bfloat16)
```

```python
import functools

import jax
import jax.numpy as jnp
from jax import lax
from jax.experimental import pallas as pl
from jax.experimental.pallas import tpu as pltpu
from jax.sharding import PartitionSpec as P

HDIM = 128
MESH = pl.DeviceIdType.MESH
neg_fill = -1e30
F32 = jnp.float32
BF16 = jnp.bfloat16
NT = (((1,), (1,)), ((), ()))
PIECES = 4


def kernel(
    kv_n, tp_n, heads, groups,
    lengths, tokens, w_query, w_key, w_value, w_gate, w_out, key_cache, value_cache, key_sum, value_sum, chosen,
    out,
    wq, wk, wv, wo, kc, vc, wide_q, scores, picked, new_k, new_v, gates,
    sbuf, rbuf, mine, obuf,
    in_sem, wq_sem, send1, recv1, send2, recv2, loc_sem,
):
    my_kv = lax.axis_index("kv")
    my_tp = lax.axis_index("tp")
    seqs, rows, width = kc.shape
    padded = wide_q.shape[1]
    per_group = heads // groups
    total = seqs * padded
    scale = HDIM ** (-0.5)
    depth = wq.shape[0]
    piece = depth // PIECES

    def query_copy(i):
        part = pl.ds(i * piece, piece)
        return pltpu.make_async_copy(w_query.at[part], wq.at[part], wq_sem.at[i])

    loads = [
        pltpu.make_async_copy(a, b, in_sem.at[i])
        for i, (a, b) in enumerate(
            ((key_cache, kc), (value_cache, vc), (w_key, wk), (w_value, wv), (w_out, wo))
        )
    ]
    for i in range(PIECES):
        query_copy(i).start()
    for load in loads:
        load.start()

    barrier = pltpu.get_barrier_semaphore()

    def each_peer(fn):
        for dt in range(tp_n):
            t = lax.rem(my_tp + dt, tp_n)

            def step(j, carry, t=t):
                fn(lax.rem(my_kv + j, kv_n), t)
                return carry

            lax.fori_loop(1 if dt == 0 else 0, kv_n, step, 0)

    each_peer(lambda k, t: pl.semaphore_signal(barrier, inc=1, device_id=(k, t), device_id_type=MESH))

    row_seq = lax.broadcasted_iota(jnp.int32, (total, 1), 0) // padded
    row_len = jnp.zeros((total, 1), jnp.int32)
    for s in range(seqs):
        row_len = jnp.where(row_seq == s, lengths[s], row_len)
    head_row = lax.broadcasted_iota(jnp.int32, (padded, 1), 0)

    def by_group(parts):
        value = parts[0]
        for g in range(1, groups):
            value = jnp.where(head_row >= g * per_group, parts[g], value)
        return value

    blocks = chosen.shape[2]
    for s in range(seqs):
        flags = chosen[s].astype(F32)
        picked[s] = by_group([jnp.broadcast_to(flags[g : g + 1], (padded, blocks)) for g in range(groups)])
    span = rows // blocks
    spread = (
        lax.broadcasted_iota(jnp.int32, (blocks, rows), 1) // span
        == lax.broadcasted_iota(jnp.int32, (blocks, rows), 0)
    ).astype(F32)
    picked_rows = jnp.dot(picked[...].reshape(total, blocks), spread, preferred_element_type=F32)
    position = my_kv * rows + lax.broadcasted_iota(jnp.int32, (total, rows), 1)
    live_sel = (picked_rows > 0.5) & (position < row_len)
    sum_rows = key_sum.shape[1]
    stride = rows // sum_rows
    col = lax.broadcasted_iota(jnp.int32, (total, seqs * sum_rows), 1)
    entry = my_kv * sum_rows + lax.rem(col, sum_rows)
    live_sum = (col // sum_rows == row_seq) & ((entry + 1) * stride <= row_len)

    queries = jnp.zeros((seqs, wq.shape[1]), F32)
    for i in range(PIECES):
        query_copy(i).wait()
        part = slice(i * piece, (i + 1) * piece)
        queries += jnp.dot(tokens[:, part], wq[part, :], preferred_element_type=F32)
    queries = queries.astype(BF16).astype(F32)
    wide_q[...] = jnp.zeros_like(wide_q)
    for h in range(heads):
        g = h // per_group
        wide_q[:, h, g * HDIM : (g + 1) * HDIM] = queries[:, h * HDIM : (h + 1) * HDIM]

    all_q = wide_q[...].reshape(total, width).astype(BF16)
    ks = key_sum[...].reshape(seqs * sum_rows, width)
    vs = value_sum[...].reshape(seqs * sum_rows, width)

    def soft(raw, live):
        raw = jnp.where(live, raw * scale, neg_fill)
        peak = jnp.max(raw, axis=-1, keepdims=True)
        weights = jnp.where(live, jnp.exp(raw - peak), 0.0)
        return peak, jnp.sum(weights, axis=-1, keepdims=True), weights

    c_peak, c_total, c_weights = soft(lax.dot_general(all_q, ks, NT, preferred_element_type=F32), live_sum)
    c_acc = jnp.dot(c_weights.astype(BF16), vs, preferred_element_type=F32).reshape(seqs, padded, width)

    loads[0].wait()
    for s in range(seqs):
        scores[s] = lax.dot_general(wide_q[s].astype(BF16), kc[s], NT, preferred_element_type=F32)
    s_peak, s_total, s_weights = soft(scores[...].reshape(total, rows), live_sel)
    scores[...] = s_weights.reshape(seqs, padded, rows)
    lane = lax.broadcasted_iota(jnp.int32, (total, HDIM), 1)
    stats = jnp.where(lane == 0, c_peak, jnp.where(lane == 1, c_total, jnp.where(lane == 2, s_peak, s_total)))
    sbuf[:, 2 * padded : 3 * padded, :] = stats.reshape(seqs, padded, HDIM)
    loads[1].wait()
    for s in range(seqs):
        acc = jnp.dot(scores[s].astype(BF16), vc[s], preferred_element_type=F32)
        sbuf[s, 0:padded, :] = by_group([c_acc[s, :, g * HDIM : (g + 1) * HDIM] for g in range(groups)])
        sbuf[s, padded : 2 * padded, :] = by_group([acc[:, g * HDIM : (g + 1) * HDIM] for g in range(groups)])

    pl.semaphore_wait(barrier, kv_n * tp_n - 1)
    owner = my_kv < seqs

    def state_copy(s, slot):
        return pltpu.make_async_remote_copy(
            src_ref=sbuf.at[s], dst_ref=rbuf.at[slot], send_sem=send1.at[s], recv_sem=recv1.at[slot],
            device_id=(s, my_tp), device_id_type=MESH,
        )

    def for_states(fn):
        @pl.when(jnp.logical_not(owner))
        def _():
            fn(lax.rem(my_kv, seqs))

        for j in range(1, seqs):
            fn(lax.rem(my_kv + j, seqs))

    for_states(lambda s: state_copy(s, my_kv).start())

    loads[2].wait()
    loads[3].wait()
    new_k[...] = jnp.dot(tokens[...], wk[...], preferred_element_type=F32).astype(BF16).astype(F32)
    new_v[...] = jnp.dot(tokens[...], wv[...], preferred_element_type=F32).astype(BF16).astype(F32)
    gates[...] = jax.nn.sigmoid(jnp.dot(tokens[...], w_gate[...], preferred_element_type=F32))

    def mixed_copy(k, t):
        return pltpu.make_async_remote_copy(
            src_ref=mine, dst_ref=obuf.at[my_tp, my_kv], send_sem=send2.at[k, t], recv_sem=recv2.at[my_tp, my_kv],
            device_id=(k, t), device_id_type=MESH,
        )

    @pl.when(owner)
    def _():
        rbuf[my_kv] = sbuf[my_kv]

        def got(j, carry):
            slot = lax.rem(my_kv + j, kv_n)
            state_copy(0, slot).wait_recv()
            return carry

        lax.fori_loop(1, kv_n, got, 0)
        chunk = min(kv_n, 16)

        def fold(first, branch):
            tile = rbuf[first : first + chunk, 2 * padded : 3 * padded, :]
            peak = tile[:, :, 2 * branch : 2 * branch + 1]
            weight = tile[:, :, 2 * branch + 1 : 2 * branch + 2]
            acc = rbuf[first : first + chunk, branch * padded : (branch + 1) * padded, :]
            top = jnp.max(peak, axis=0)
            factor = jnp.exp(peak - top[None])
            return top, jnp.sum(weight * factor, axis=0), jnp.sum(acc * factor, axis=0)

        def merge(a, b):
            top = jnp.maximum(a[0], b[0])
            fa, fb = jnp.exp(a[0] - top), jnp.exp(b[0] - top)
            return top, a[1] * fa + b[1] * fb, a[2] * fa + b[2] * fb

        states = []
        for branch in range(2):
            state = fold(0, branch)
            for first in range(chunk, kv_n, chunk):
                state = merge(state, fold(first, branch))
            states.append(state)
        compressed = states[0][2] / states[0][1]
        my_q = wide_q[my_kv]
        my_k = new_k[pl.ds(my_kv, 1), :]
        my_v = new_v[pl.ds(my_kv, 1), :]
        own_score = jnp.sum(my_q * my_k, axis=-1, keepdims=True) * scale
        own_value = by_group(
            [jnp.broadcast_to(my_v[:, g * HDIM : (g + 1) * HDIM], (padded, HDIM)) for g in range(groups)]
        )
        _, weight, acc = merge(states[1], (own_score, jnp.ones_like(own_score), own_value))
        selected = acc / weight
        my_gates = gates[pl.ds(my_kv, 1), :]
        gate_col = lax.broadcasted_iota(jnp.int32, (padded, my_gates.shape[1]), 1)
        first_col = 2 * (my_tp * heads + head_row)

        def gate(branch):
            hit = gate_col == first_col + branch
            return jnp.sum(jnp.where(hit, my_gates, 0.0), axis=-1, keepdims=True)

        mixed = gate(0) * compressed + gate(1) * selected
        mixed = mixed.astype(BF16).astype(F32)
        mine[...] = mixed
        obuf[my_tp, my_kv] = mixed
        each_peer(lambda k, t: mixed_copy(k, t).start())

    loads[4].wait()
    for t in range(tp_n):
        for s in range(seqs):

            @pl.when(jnp.logical_or(my_tp != t, my_kv != s))
            def _():
                pltpu.make_async_remote_copy(
                    src_ref=mine, dst_ref=obuf.at[t, s], send_sem=send2.at[0, 0], recv_sem=recv2.at[t, s],
                    device_id=(my_kv, my_tp), device_id_type=MESH,
                ).wait_recv()

    mixed_all = jnp.concatenate(
        [obuf[t, :, h, :] for t in range(tp_n) for h in range(heads)], axis=1
    ).astype(BF16)
    out[...] = jnp.dot(mixed_all, wo[...], preferred_element_type=F32).astype(BF16)

    for_states(lambda s: state_copy(s, my_kv).wait_send())

    @pl.when(owner)
    def _():
        each_peer(lambda k, t: mixed_copy(k, t).wait_send())


def solution(mesh):
    kv_n, tp_n = mesh.shape["kv"], mesh.shape["tp"]

    def local(
        tokens, w_query, w_key, w_value, w_gate, w_out, key_cache, value_cache, key_sum, value_sum, lengths, chosen
    ):
        seqs, rows, width = key_cache.shape
        heads, groups = w_query.shape[1] // HDIM, w_key.shape[1] // HDIM
        padded = -(-heads // 8) * 8
        assert kv_n >= seqs
        vmem = pl.BlockSpec(memory_space=pltpu.VMEM)
        hbm = pl.BlockSpec(memory_space=pl.ANY)
        smem = pl.BlockSpec(memory_space=pltpu.SMEM)
        dma = pltpu.SemaphoreType.DMA
        return pl.pallas_call(
            functools.partial(kernel, kv_n, tp_n, heads, groups),
            out_shape=jax.ShapeDtypeStruct((seqs, w_out.shape[1]), BF16),
            in_specs=[smem, vmem, hbm, hbm, hbm, vmem, hbm, hbm, hbm, vmem, vmem, vmem],
            out_specs=vmem,
            scratch_shapes=[
                pltpu.VMEM(w_query.shape, BF16),
                pltpu.VMEM(w_key.shape, BF16),
                pltpu.VMEM(w_value.shape, BF16),
                pltpu.VMEM(w_out.shape, BF16),
                pltpu.VMEM(key_cache.shape, BF16),
                pltpu.VMEM(value_cache.shape, BF16),
                pltpu.VMEM((seqs, padded, width), F32),
                pltpu.VMEM((seqs, padded, rows), F32),
                pltpu.VMEM((seqs, padded, chosen.shape[2]), F32),
                pltpu.VMEM((seqs, width), F32),
                pltpu.VMEM((seqs, width), F32),
                pltpu.VMEM((seqs, w_gate.shape[1]), F32),
                pltpu.VMEM((seqs, 3 * padded, HDIM), F32),
                pltpu.VMEM((kv_n, 3 * padded, HDIM), F32),
                pltpu.VMEM((padded, HDIM), F32),
                pltpu.VMEM((tp_n, seqs, padded, HDIM), F32),
                dma((5,)),
                dma((PIECES,)),
                dma((seqs,)),
                dma((kv_n,)),
                dma((kv_n, tp_n)),
                dma((tp_n, seqs)),
                dma((1,)),
            ],
            compiler_params=pltpu.CompilerParams(collective_id=0, has_side_effects=True),
            name="decode",
        )(lengths, tokens, w_query, w_key, w_value, w_gate, w_out, key_cache, value_cache, key_sum, value_sum, chosen)

    return jax.shard_map(
        local,
        mesh=mesh,
        in_specs=(
            P(),
            P(None, "tp"),
            P(None, "tp"),
            P(None, "tp"),
            P(),
            P(None, "tp"),
            P(None, "kv", "tp"),
            P(None, "kv", "tp"),
            P(None, "kv", "tp"),
            P(None, "kv", "tp"),
            P(),
            P(None, "tp", "kv"),
        ),
        out_specs=P(None, "tp"),
        check_vma=False,
    )
```

```python
import functools

import jax
import jax.numpy as jnp
from jax import lax
from jax.experimental import pallas as pl
from jax.experimental.pallas import tpu as pltpu
from jax.sharding import PartitionSpec as P

HDIM = 128
MESH = pl.DeviceIdType.MESH
neg_fill = -1e30
F32 = jnp.float32
BF16 = jnp.bfloat16
NT = (((1,), (1,)), ((), ()))
PIECES = 4


def kernel(
    kv_n, tp_n, heads, groups,
    lengths, tokens_in, w_query, w_key, w_value, w_gate_in, w_out, key_cache, value_cache, key_in, value_in, chosen_in,
    out,
    tokens, w_gate, key_sum, value_sum, chosen, heads_f32,
    wq, wk, wv, wo, kc, vc, wide_q, scores, new_k, new_v, gates,
    sbuf, rbuf, mine, obuf,
    in_sem, wq_sem, send1, recv1, send2, recv2,
):
    my_kv = lax.axis_index("kv")
    my_tp = lax.axis_index("tp")
    seqs, rows, width = kc.shape
    padded = wide_q.shape[1]
    per_group = heads // groups
    total = seqs * padded
    scale = HDIM ** (-0.5)
    depth = wq.shape[0]
    piece = depth // PIECES

    def query_copy(i):
        part = pl.ds(i * piece, piece)
        return pltpu.make_async_copy(w_query.at[part], wq.at[part], wq_sem.at[i])

    loads = [
        pltpu.make_async_copy(a, b, in_sem.at[i])
        for i, (a, b) in enumerate(
            (
                (key_cache, kc), (value_cache, vc), (w_key, wk), (w_value, wv), (w_out, wo),
                (tokens_in, tokens), (chosen_in, chosen), (key_in, key_sum), (value_in, value_sum), (w_gate_in, w_gate),
            )
        )
    ]
    loads[5].start()
    loads[6].start()
    for i in range(PIECES):
        query_copy(i).start()
    for i in (7, 8, 0, 1, 2, 3, 9, 4):
        loads[i].start()

    barrier = pltpu.get_barrier_semaphore()

    def each_peer(fn):
        for dt in range(tp_n):
            t = lax.rem(my_tp + dt, tp_n)

            def step(j, carry, t=t):
                fn(lax.rem(my_kv + j, kv_n), t)
                return carry

            lax.fori_loop(1 if dt == 0 else 0, kv_n, step, 0)

    each_peer(lambda k, t: pl.semaphore_signal(barrier, inc=1, device_id=(k, t), device_id_type=MESH))

    row_seq = lax.broadcasted_iota(jnp.int32, (total, 1), 0) // padded
    row_len = jnp.zeros((total, 1), jnp.int32)
    for s in range(seqs):
        row_len = jnp.where(row_seq == s, lengths[s], row_len)
    head_row = lax.broadcasted_iota(jnp.int32, (padded, 1), 0)

    def by_group(parts):
        value = parts[0]
        for g in range(1, groups):
            value = jnp.where(head_row >= g * per_group, parts[g], value)
        return value

    blocks = chosen.shape[1]
    span = rows // blocks
    spread = (
        lax.broadcasted_iota(jnp.int32, (blocks, rows), 1) // span
        == lax.broadcasted_iota(jnp.int32, (blocks, rows), 0)
    ).astype(F32)
    to_row = lax.broadcasted_iota(jnp.int32, (seqs, total), 1)
    same_seq = to_row // padded == lax.broadcasted_iota(jnp.int32, (seqs, total), 0)
    row_group = jnp.minimum(lax.rem(to_row, padded) // per_group, groups - 1)
    loads[6].wait()
    flags = jnp.zeros((blocks, total), F32)
    for g in range(groups):
        place = (same_seq & (row_group == g)).astype(F32)
        flags += jnp.dot(chosen[g].astype(F32), place, preferred_element_type=F32)
    picked_rows = lax.dot_general(flags, spread, (((0,), (0,)), ((), ())), preferred_element_type=F32)
    position = my_kv * rows + lax.broadcasted_iota(jnp.int32, (total, rows), 1)
    live_sel = (picked_rows > 0.5) & (position < row_len)
    sum_rows = key_sum.shape[1]
    stride = rows // sum_rows
    col = lax.broadcasted_iota(jnp.int32, (total, seqs * sum_rows), 1)
    entry = my_kv * sum_rows + lax.rem(col, sum_rows)
    live_sum = (col // sum_rows == row_seq) & ((entry + 1) * stride <= row_len)

    loads[5].wait()
    queries = jnp.zeros((seqs, wq.shape[1]), F32)
    for i in range(PIECES):
        query_copy(i).wait()
        part = slice(i * piece, (i + 1) * piece)
        queries += jnp.dot(tokens[:, part], wq[part, :], preferred_element_type=F32)
    queries = queries.astype(BF16).astype(F32)
    wide_q[...] = jnp.zeros_like(wide_q)
    for h in range(heads):
        g = h // per_group
        wide_q[:, h, g * HDIM : (g + 1) * HDIM] = queries[:, h * HDIM : (h + 1) * HDIM]

    all_q = wide_q[...].reshape(total, width).astype(BF16)
    loads[7].wait()
    loads[8].wait()
    ks = key_sum[...].reshape(seqs * sum_rows, width)
    vs = value_sum[...].reshape(seqs * sum_rows, width)

    def soft(raw, live):
        raw = jnp.where(live, raw * scale, neg_fill)
        peak = jnp.max(raw, axis=-1, keepdims=True)
        weights = jnp.where(live, jnp.exp(raw - peak), 0.0)
        return peak, jnp.sum(weights, axis=-1, keepdims=True), weights

    c_peak, c_total, c_weights = soft(lax.dot_general(all_q, ks, NT, preferred_element_type=F32), live_sum)
    c_acc = jnp.dot(c_weights.astype(BF16), vs, preferred_element_type=F32).reshape(seqs, padded, width)

    loads[0].wait()
    for s in range(seqs):
        scores[s] = lax.dot_general(wide_q[s].astype(BF16), kc[s], NT, preferred_element_type=F32)
    s_peak, s_total, s_weights = soft(scores[...].reshape(total, rows), live_sel)
    scores[...] = s_weights.reshape(seqs, padded, rows)
    lane = lax.broadcasted_iota(jnp.int32, (total, HDIM), 1)
    which = lax.rem(lane, 4)
    stats = jnp.where(which == 0, c_peak, jnp.where(which == 1, c_total, jnp.where(which == 2, s_peak, s_total)))
    high = stats.astype(BF16).astype(F32)
    rest = stats - high
    middle = rest.astype(BF16).astype(F32)
    stats = jnp.where(lane < 4, high, jnp.where(lane < 8, middle, rest - middle)).reshape(seqs, padded, HDIM)
    loads[1].wait()
    for s in range(seqs):
        acc = jnp.dot(scores[s].astype(BF16), vc[s], preferred_element_type=F32)
        sbuf[s] = jnp.concatenate(
            [
                by_group([c_acc[s, :, g * HDIM : (g + 1) * HDIM] for g in range(groups)]),
                by_group([acc[:, g * HDIM : (g + 1) * HDIM] for g in range(groups)]),
                stats[s],
            ],
            axis=0,
        ).astype(BF16)

    pl.semaphore_wait(barrier, kv_n * tp_n - 1)
    my_seq = lax.div(my_kv * seqs + (kv_n - 1), kv_n)
    owner = lax.div(my_seq * kv_n, seqs) == my_kv

    def state_copy(s, slot):
        return pltpu.make_async_remote_copy(
            src_ref=sbuf.at[s], dst_ref=rbuf.at[slot], send_sem=send1.at[s], recv_sem=recv1.at[slot],
            device_id=(lax.div(s * kv_n, seqs), my_tp), device_id_type=MESH,
        )

    def for_states(fn):
        @pl.when(jnp.logical_not(owner))
        def _():
            fn(lax.rem(my_seq, seqs))

        for j in range(1, seqs):
            fn(lax.rem(my_seq + j, seqs))

    for_states(lambda s: state_copy(s, my_kv).start())

    loads[2].wait()
    loads[3].wait()
    loads[9].wait()
    new_k[...] = jnp.dot(tokens[...], wk[...], preferred_element_type=F32).astype(BF16).astype(F32)
    new_v[...] = jnp.dot(tokens[...], wv[...], preferred_element_type=F32).astype(BF16).astype(F32)
    gates[...] = jax.nn.sigmoid(lax.dot_general(tokens[...], w_gate[...], NT, preferred_element_type=F32))

    def mixed_copy(k, t):
        return pltpu.make_async_remote_copy(
            src_ref=mine, dst_ref=obuf.at[my_tp, my_seq], send_sem=send2.at[k, t], recv_sem=recv2.at[my_tp, my_seq],
            device_id=(k, t), device_id_type=MESH,
        )

    @pl.when(owner)
    def _():
        rbuf[my_kv] = sbuf[my_seq]

        def got(j, carry):
            slot = lax.rem(my_kv + j, kv_n)
            state_copy(0, slot).wait_recv()
            return carry

        lax.fori_loop(1, kv_n, got, 0)
        chunk = min(kv_n, 16)

        def fold(first, branch):
            block = rbuf[first : first + chunk].astype(F32)
            tile = block[:, 2 * padded : 3 * padded, 0:12]
            tile = tile[:, :, 0:4] + tile[:, :, 4:8] + tile[:, :, 8:12]
            peak = tile[:, :, 2 * branch : 2 * branch + 1]
            weight = tile[:, :, 2 * branch + 1 : 2 * branch + 2]
            acc = block[:, branch * padded : (branch + 1) * padded, :]
            top = jnp.max(peak, axis=0)
            factor = jnp.exp(peak - top[None])
            return top, jnp.sum(weight * factor, axis=0), jnp.sum(acc * factor, axis=0)

        def merge(a, b):
            top = jnp.maximum(a[0], b[0])
            fa, fb = jnp.exp(a[0] - top), jnp.exp(b[0] - top)
            return top, a[1] * fa + b[1] * fb, a[2] * fa + b[2] * fb

        states = []
        for branch in range(2):
            state = fold(0, branch)
            for first in range(chunk, kv_n, chunk):
                state = merge(state, fold(first, branch))
            states.append(state)
        compressed = states[0][2] / states[0][1]
        my_q = wide_q[my_seq]
        my_k = new_k[pl.ds(my_seq, 1), :]
        my_v = new_v[pl.ds(my_seq, 1), :]
        own_score = jnp.sum(my_q * my_k, axis=-1, keepdims=True) * scale
        own_value = by_group(
            [jnp.broadcast_to(my_v[:, g * HDIM : (g + 1) * HDIM], (padded, HDIM)) for g in range(groups)]
        )
        _, weight, acc = merge(states[1], (own_score, jnp.ones_like(own_score), own_value))
        selected = acc / weight
        my_gates = gates[pl.ds(my_seq, 1), :]
        gate_col = lax.broadcasted_iota(jnp.int32, (padded, my_gates.shape[1]), 1)
        first_col = 2 * (my_tp * heads + head_row)

        def gate(branch):
            hit = gate_col == first_col + branch
            return jnp.sum(jnp.where(hit, my_gates, 0.0), axis=-1, keepdims=True)

        mixed = gate(0) * compressed + gate(1) * selected
        mixed = mixed.astype(BF16)
        mine[...] = mixed
        obuf[my_tp, my_seq] = mixed
        each_peer(lambda k, t: mixed_copy(k, t).start())

    loads[4].wait()
    for t in range(tp_n):
        for s in range(seqs):

            @pl.when(jnp.logical_or(my_tp != t, my_kv != s * kv_n // seqs))
            def _():
                pltpu.make_async_remote_copy(
                    src_ref=mine, dst_ref=obuf.at[t, s], send_sem=send2.at[0, 0], recv_sem=recv2.at[t, s],
                    device_id=(my_kv, my_tp), device_id_type=MESH,
                ).wait_recv()

    heads_f32[...] = obuf[...].astype(F32)
    mixed_all = jnp.concatenate(
        [heads_f32[t, :, h, :] for t in range(tp_n) for h in range(heads)], axis=1
    ).astype(BF16)
    out[...] = jnp.dot(mixed_all, wo[...], preferred_element_type=F32).astype(BF16)

    for_states(lambda s: state_copy(s, my_kv).wait_send())

    @pl.when(owner)
    def _():
        each_peer(lambda k, t: mixed_copy(k, t).wait_send())


def solution(mesh):
    kv_n, tp_n = mesh.shape["kv"], mesh.shape["tp"]

    def local(
        tokens, w_query, w_key, w_value, w_gate, w_out, key_cache, value_cache, key_sum, value_sum, lengths, chosen
    ):
        seqs, rows, width = key_cache.shape
        heads, groups = w_query.shape[1] // HDIM, w_key.shape[1] // HDIM
        padded = -(-heads // 8) * 8
        assert kv_n >= seqs
        vmem = pl.BlockSpec(memory_space=pltpu.VMEM)
        hbm = pl.BlockSpec(memory_space=pl.ANY)
        smem = pl.BlockSpec(memory_space=pltpu.SMEM)
        dma = pltpu.SemaphoreType.DMA
        return pl.pallas_call(
            functools.partial(kernel, kv_n, tp_n, heads, groups),
            out_shape=jax.ShapeDtypeStruct((seqs, w_out.shape[1]), BF16),
            in_specs=[smem] + [hbm] * 11,
            out_specs=vmem,
            scratch_shapes=[
                pltpu.VMEM(tokens.shape, BF16),
                pltpu.VMEM(w_gate.shape[::-1], BF16),
                pltpu.VMEM(key_sum.shape, BF16),
                pltpu.VMEM(value_sum.shape, BF16),
                pltpu.VMEM((groups, chosen.shape[2], seqs), jnp.int32),
                pltpu.VMEM((tp_n, seqs, padded, HDIM), F32),
                pltpu.VMEM(w_query.shape, BF16),
                pltpu.VMEM(w_key.shape, BF16),
                pltpu.VMEM(w_value.shape, BF16),
                pltpu.VMEM(w_out.shape, BF16),
                pltpu.VMEM(key_cache.shape, BF16),
                pltpu.VMEM(value_cache.shape, BF16),
                pltpu.VMEM((seqs, padded, width), F32),
                pltpu.VMEM((seqs, padded, rows), F32),
                pltpu.VMEM((seqs, width), F32),
                pltpu.VMEM((seqs, width), F32),
                pltpu.VMEM((seqs, w_gate.shape[1]), F32),
                pltpu.VMEM((seqs, 3 * padded, HDIM), BF16),
                pltpu.VMEM((kv_n, 3 * padded, HDIM), BF16),
                pltpu.VMEM((padded, HDIM), BF16),
                pltpu.VMEM((tp_n, seqs, padded, HDIM), BF16),
                dma((10,)),
                dma((PIECES,)),
                dma((seqs,)),
                dma((kv_n,)),
                dma((kv_n, tp_n)),
                dma((tp_n, seqs)),
            ],
            compiler_params=pltpu.CompilerParams(collective_id=0, has_side_effects=True),
            name="decode",
        )(
            lengths, tokens, w_query, w_key, w_value, w_gate.T, w_out, key_cache, value_cache, key_sum, value_sum,
            jnp.transpose(chosen, (1, 2, 0)),
        )

    return jax.shard_map(
        local,
        mesh=mesh,
        in_specs=(
            P(),
            P(None, "tp"),
            P(None, "tp"),
            P(None, "tp"),
            P(),
            P(None, "tp"),
            P(None, "kv", "tp"),
            P(None, "kv", "tp"),
            P(None, "kv", "tp"),
            P(None, "kv", "tp"),
            P(),
            P(None, "tp", "kv"),
        ),
        out_specs=P(None, "tp"),
        check_vma=False,
    )
```

```python
import functools

import jax
import jax.numpy as jnp
from jax import lax
from jax.experimental import pallas as pl
from jax.experimental.pallas import tpu as pltpu
from jax.sharding import PartitionSpec as P

HDIM = 128
MESH = pl.DeviceIdType.MESH
neg_fill = -1e30
F32 = jnp.float32
BF16 = jnp.bfloat16
NT = (((1,), (1,)), ((), ()))
PIECES = 4


def kernel(
    kv_n, tp_n, heads, groups,
    lengths, tokens_in, w_query, w_key, w_value, w_gate_in, w_out, key_cache, value_cache, key_in, value_in, chosen_in,
    out,
    tokens, w_gate, key_sum, value_sum, chosen, heads_f32,
    wq, wk, wv, wo, kc, vc, wide_q, scores, new_k, new_v, gates,
    sbuf, rbuf, mine, obuf,
    in_sem, wq_sem, send1, recv1, send2, recv2,
):
    my_kv = lax.axis_index("kv")
    my_tp = lax.axis_index("tp")
    seqs, rows, width = kc.shape
    padded = wide_q.shape[1]
    per_group = heads // groups
    total = seqs * padded
    scale = HDIM ** (-0.5)
    depth = wq.shape[0]
    piece = depth // PIECES

    def query_copy(i):
        part = pl.ds(i * piece, piece)
        return pltpu.make_async_copy(w_query.at[part], wq.at[part], wq_sem.at[i])

    loads = [
        pltpu.make_async_copy(a, b, in_sem.at[i])
        for i, (a, b) in enumerate(
            (
                (key_cache, kc), (value_cache, vc), (w_key, wk), (w_value, wv), (w_out, wo),
                (tokens_in, tokens), (chosen_in, chosen), (key_in, key_sum), (value_in, value_sum), (w_gate_in, w_gate),
            )
        )
    ]
    loads[5].start()
    loads[6].start()
    for i in range(PIECES):
        query_copy(i).start()
    for i in (7, 8, 0, 1, 2, 3, 9, 4):
        loads[i].start()

    barrier = pltpu.get_barrier_semaphore()

    def each_peer(fn, straight=kv_n <= 16):
        for dt in range(tp_n):
            t = lax.rem(my_tp + dt, tp_n)

            def step(j, carry, t=t):
                fn(lax.rem(my_kv + j, kv_n), t)
                return carry

            first = 1 if dt == 0 else 0
            if straight:
                for j in range(first, kv_n):
                    step(j, 0)
            else:
                lax.fori_loop(first, kv_n, step, 0)

    each_peer(lambda k, t: pl.semaphore_signal(barrier, inc=1, device_id=(k, t), device_id_type=MESH))

    row_seq = lax.broadcasted_iota(jnp.int32, (total, 1), 0) // padded
    row_len = jnp.zeros((total, 1), jnp.int32)
    for s in range(seqs):
        row_len = jnp.where(row_seq == s, lengths[s], row_len)
    head_row = lax.broadcasted_iota(jnp.int32, (padded, 1), 0)

    def by_group(parts):
        value = parts[0]
        for g in range(1, groups):
            value = jnp.where(head_row >= g * per_group, parts[g], value)
        return value

    blocks = chosen.shape[1]
    span = rows // blocks
    spread = (
        lax.broadcasted_iota(jnp.int32, (blocks, rows), 1) // span
        == lax.broadcasted_iota(jnp.int32, (blocks, rows), 0)
    ).astype(F32)
    to_row = lax.broadcasted_iota(jnp.int32, (seqs, total), 1)
    same_seq = to_row // padded == lax.broadcasted_iota(jnp.int32, (seqs, total), 0)
    row_group = jnp.minimum(lax.rem(to_row, padded) // per_group, groups - 1)
    loads[6].wait()
    flags = jnp.zeros((blocks, total), F32)
    for g in range(groups):
        place = (same_seq & (row_group == g)).astype(F32)
        flags += jnp.dot(chosen[g].astype(F32), place, preferred_element_type=F32)
    picked_rows = lax.dot_general(flags, spread, (((0,), (0,)), ((), ())), preferred_element_type=F32)
    position = my_kv * rows + lax.broadcasted_iota(jnp.int32, (total, rows), 1)
    live_sel = (picked_rows > 0.5) & (position < row_len)
    sum_rows = key_sum.shape[1]
    stride = rows // sum_rows
    col = lax.broadcasted_iota(jnp.int32, (total, seqs * sum_rows), 1)
    entry = my_kv * sum_rows + lax.rem(col, sum_rows)
    live_sum = (col // sum_rows == row_seq) & ((entry + 1) * stride <= row_len)

    loads[5].wait()
    queries = jnp.zeros((seqs, wq.shape[1]), F32)
    for i in range(PIECES):
        query_copy(i).wait()
        part = slice(i * piece, (i + 1) * piece)
        queries += jnp.dot(tokens[:, part], wq[part, :], preferred_element_type=F32)
    queries = queries.astype(BF16).astype(F32)
    wide_q[...] = jnp.zeros_like(wide_q)
    for h in range(heads):
        g = h // per_group
        wide_q[:, h, g * HDIM : (g + 1) * HDIM] = queries[:, h * HDIM : (h + 1) * HDIM]

    all_q = wide_q[...].reshape(total, width).astype(BF16)
    loads[7].wait()
    loads[8].wait()
    ks = key_sum[...].reshape(seqs * sum_rows, width)
    vs = value_sum[...].reshape(seqs * sum_rows, width)

    def soft(raw, live):
        raw = jnp.where(live, raw * scale, neg_fill)
        peak = jnp.max(raw, axis=-1, keepdims=True)
        weights = jnp.where(live, jnp.exp(raw - peak), 0.0)
        return peak, jnp.sum(weights, axis=-1, keepdims=True), weights

    c_peak, c_total, c_weights = soft(lax.dot_general(all_q, ks, NT, preferred_element_type=F32), live_sum)
    c_acc = jnp.dot(c_weights.astype(BF16), vs, preferred_element_type=F32).reshape(seqs, padded, width)

    loads[0].wait()
    for s in range(seqs):
        scores[s] = lax.dot_general(wide_q[s].astype(BF16), kc[s], NT, preferred_element_type=F32)
    s_peak, s_total, s_weights = soft(scores[...].reshape(total, rows), live_sel)
    scores[...] = s_weights.reshape(seqs, padded, rows)
    lane = lax.broadcasted_iota(jnp.int32, (total, HDIM), 1)
    which = lax.rem(lane, 4)
    stats = jnp.where(which == 0, c_peak, jnp.where(which == 1, c_total, jnp.where(which == 2, s_peak, s_total)))
    high = stats.astype(BF16).astype(F32)
    rest = stats - high
    middle = rest.astype(BF16).astype(F32)
    stats = jnp.where(lane < 4, high, jnp.where(lane < 8, middle, rest - middle)).reshape(seqs, padded, HDIM)
    loads[1].wait()
    for s in range(seqs):
        acc = jnp.dot(scores[s].astype(BF16), vc[s], preferred_element_type=F32)
        sbuf[s] = jnp.concatenate(
            [
                by_group([c_acc[s, :, g * HDIM : (g + 1) * HDIM] for g in range(groups)]),
                by_group([acc[:, g * HDIM : (g + 1) * HDIM] for g in range(groups)]),
                stats[s],
            ],
            axis=0,
        ).astype(BF16)

    pl.semaphore_wait(barrier, kv_n * tp_n - 1)
    my_seq = lax.div(my_kv * seqs + (kv_n - 1), kv_n)
    owner = lax.div(my_seq * kv_n, seqs) == my_kv

    def state_copy(s, slot):
        return pltpu.make_async_remote_copy(
            src_ref=sbuf.at[s], dst_ref=rbuf.at[slot], send_sem=send1.at[s], recv_sem=recv1.at[slot],
            device_id=(lax.div(s * kv_n, seqs), my_tp), device_id_type=MESH,
        )

    def for_states(fn):
        @pl.when(jnp.logical_not(owner))
        def _():
            fn(lax.rem(my_seq, seqs))

        for j in range(1, seqs):
            fn(lax.rem(my_seq + j, seqs))

    for_states(lambda s: state_copy(s, my_kv).start())

    loads[2].wait()
    loads[3].wait()
    loads[9].wait()
    new_k[...] = jnp.dot(tokens[...], wk[...], preferred_element_type=F32).astype(BF16).astype(F32)
    new_v[...] = jnp.dot(tokens[...], wv[...], preferred_element_type=F32).astype(BF16).astype(F32)
    gates[...] = jax.nn.sigmoid(lax.dot_general(tokens[...], w_gate[...], NT, preferred_element_type=F32))

    def mixed_copy(k, t):
        return pltpu.make_async_remote_copy(
            src_ref=mine, dst_ref=obuf.at[my_tp, my_seq], send_sem=send2.at[k, t], recv_sem=recv2.at[my_tp, my_seq],
            device_id=(k, t), device_id_type=MESH,
        )

    @pl.when(owner)
    def _():
        rbuf[my_kv] = sbuf[my_seq]

        my_q = wide_q[my_seq]
        my_k = new_k[pl.ds(my_seq, 1), :]
        my_v = new_v[pl.ds(my_seq, 1), :]
        own_score = jnp.sum(my_q * my_k, axis=-1, keepdims=True) * scale
        own_value = by_group(
            [jnp.broadcast_to(my_v[:, g * HDIM : (g + 1) * HDIM], (padded, HDIM)) for g in range(groups)]
        )
        my_gates = gates[pl.ds(my_seq, 1), :]
        gate_col = lax.broadcasted_iota(jnp.int32, (padded, my_gates.shape[1]), 1)
        first_col = 2 * (my_tp * heads + head_row)

        def gate(branch):
            hit = gate_col == first_col + branch
            return jnp.sum(jnp.where(hit, my_gates, 0.0), axis=-1, keepdims=True)

        gate_c, gate_s = gate(0), gate(1)

        def got(j, carry):
            slot = lax.rem(my_kv + j, kv_n)
            state_copy(0, slot).wait_recv()
            return carry

        lax.fori_loop(1, kv_n, got, 0)
        chunk = min(kv_n, 16)

        def fold(first, branch):
            block = rbuf[first : first + chunk].astype(F32)
            tile = block[:, 2 * padded : 3 * padded, 0:12]
            tile = tile[:, :, 0:4] + tile[:, :, 4:8] + tile[:, :, 8:12]
            peak = tile[:, :, 2 * branch : 2 * branch + 1]
            weight = tile[:, :, 2 * branch + 1 : 2 * branch + 2]
            acc = block[:, branch * padded : (branch + 1) * padded, :]
            top = jnp.max(peak, axis=0)
            factor = jnp.exp(peak - top[None])
            return top, jnp.sum(weight * factor, axis=0), jnp.sum(acc * factor, axis=0)

        def merge(a, b):
            top = jnp.maximum(a[0], b[0])
            fa, fb = jnp.exp(a[0] - top), jnp.exp(b[0] - top)
            return top, a[1] * fa + b[1] * fb, a[2] * fa + b[2] * fb

        states = []
        for branch in range(2):
            state = fold(0, branch)
            for first in range(chunk, kv_n, chunk):
                state = merge(state, fold(first, branch))
            states.append(state)
        compressed = states[0][2] / states[0][1]
        _, weight, acc = merge(states[1], (own_score, jnp.ones_like(own_score), own_value))
        selected = acc / weight
        mixed = gate_c * compressed + gate_s * selected
        mixed = mixed.astype(BF16)
        mine[...] = mixed
        obuf[my_tp, my_seq] = mixed
        each_peer(lambda k, t: mixed_copy(k, t).start())

    for_states(lambda s: state_copy(s, my_kv).wait_send())

    @pl.when(owner)
    def _():
        each_peer(lambda k, t: mixed_copy(k, t).wait_send(), False)

    loads[4].wait()
    for t in range(tp_n):
        for s in range(seqs):

            @pl.when(jnp.logical_or(my_tp != t, my_kv != s * kv_n // seqs))
            def _():
                pltpu.make_async_remote_copy(
                    src_ref=mine, dst_ref=obuf.at[t, s], send_sem=send2.at[0, 0], recv_sem=recv2.at[t, s],
                    device_id=(my_kv, my_tp), device_id_type=MESH,
                ).wait_recv()

    heads_f32[...] = obuf[...].astype(F32)
    mixed_all = jnp.concatenate(
        [heads_f32[t, :, h, :] for t in range(tp_n) for h in range(heads)], axis=1
    ).astype(BF16)
    out[...] = jnp.dot(mixed_all, wo[...], preferred_element_type=F32).astype(BF16)


def solution(mesh):
    kv_n, tp_n = mesh.shape["kv"], mesh.shape["tp"]

    def local(
        tokens, w_query, w_key, w_value, w_gate, w_out, key_cache, value_cache, key_sum, value_sum, lengths, chosen
    ):
        seqs, rows, width = key_cache.shape
        heads, groups = w_query.shape[1] // HDIM, w_key.shape[1] // HDIM
        padded = -(-heads // 8) * 8
        assert kv_n >= seqs
        vmem = pl.BlockSpec(memory_space=pltpu.VMEM)
        hbm = pl.BlockSpec(memory_space=pl.ANY)
        smem = pl.BlockSpec(memory_space=pltpu.SMEM)
        dma = pltpu.SemaphoreType.DMA
        return pl.pallas_call(
            functools.partial(kernel, kv_n, tp_n, heads, groups),
            out_shape=jax.ShapeDtypeStruct((seqs, w_out.shape[1]), BF16),
            in_specs=[smem] + [hbm] * 11,
            out_specs=vmem,
            scratch_shapes=[
                pltpu.VMEM(tokens.shape, BF16),
                pltpu.VMEM(w_gate.shape[::-1], BF16),
                pltpu.VMEM(key_sum.shape, BF16),
                pltpu.VMEM(value_sum.shape, BF16),
                pltpu.VMEM((groups, chosen.shape[2], seqs), jnp.int32),
                pltpu.VMEM((tp_n, seqs, padded, HDIM), F32),
                pltpu.VMEM(w_query.shape, BF16),
                pltpu.VMEM(w_key.shape, BF16),
                pltpu.VMEM(w_value.shape, BF16),
                pltpu.VMEM(w_out.shape, BF16),
                pltpu.VMEM(key_cache.shape, BF16),
                pltpu.VMEM(value_cache.shape, BF16),
                pltpu.VMEM((seqs, padded, width), F32),
                pltpu.VMEM((seqs, padded, rows), F32),
                pltpu.VMEM((seqs, width), F32),
                pltpu.VMEM((seqs, width), F32),
                pltpu.VMEM((seqs, w_gate.shape[1]), F32),
                pltpu.VMEM((seqs, 3 * padded, HDIM), BF16),
                pltpu.VMEM((kv_n, 3 * padded, HDIM), BF16),
                pltpu.VMEM((padded, HDIM), BF16),
                pltpu.VMEM((tp_n, seqs, padded, HDIM), BF16),
                dma((10,)),
                dma((PIECES,)),
                dma((seqs,)),
                dma((kv_n,)),
                dma((kv_n, tp_n)),
                dma((tp_n, seqs)),
            ],
            compiler_params=pltpu.CompilerParams(collective_id=0, has_side_effects=True),
            name="decode",
        )(
            lengths, tokens, w_query, w_key, w_value, w_gate.T, w_out, key_cache, value_cache, key_sum, value_sum,
            jnp.transpose(chosen, (1, 2, 0)),
        )

    return jax.shard_map(
        local,
        mesh=mesh,
        in_specs=(
            P(),
            P(None, "tp"),
            P(None, "tp"),
            P(None, "tp"),
            P(),
            P(None, "tp"),
            P(None, "kv", "tp"),
            P(None, "kv", "tp"),
            P(None, "kv", "tp"),
            P(None, "kv", "tp"),
            P(),
            P(None, "tp", "kv"),
        ),
        out_specs=P(None, "tp"),
        check_vma=False,
    )
```
